128 devices in a mesh: ep: 32 (over z, y, core), tp: 4 (over x).
Axes of the slice: x: 4, y: 4, z: 4, core: 2. Of those that a mesh axis runs over, the one named last changes fastest.
Arguments:
- value_in: bfloat16 [16384, 1024], P('ep', 'tp'), may hold values from -6 to 6
- gate_in: bfloat16 [16384, 1024], P('ep', 'tp'), may hold values from -6 to 6
- outer_gate: bfloat16 [16384, 1024], P('ep', 'tp'), may hold values from -6 to 6
- conv_weight: bfloat16 [3, 1024], P(None, 'tp'), may hold values from -3.5 to 3.5
- out_weight: bfloat16 [1024, 2048], P('tp'), may hold values from -0.1875 to 0.1875
- moe_tokens: bfloat16 [16384, 2048], P(('ep', 'tp')), may hold values from -6 to 6
- norm_gain: bfloat16 [2048], replicated, may hold values from 0.099609375 to 1.8984375
- routes: int32 [16384, 2], P(('ep', 'tp')), may hold values from 0 to 31, all different within a row; in each aligned block of 128 rows (0 to 127, 128 to 255, ...) at most 12 rows name the same one
- route_weight: float32 [16384, 2], P(('ep', 'tp')), may hold values from 0.1 to 1
- expert_gate: bfloat16 [32, 2048, 6144], P('ep', None, 'tp'), may hold values from -0.125 to 0.125
- expert_up: bfloat16 [32, 2048, 6144], P('ep', None, 'tp'), may hold values from -0.125 to 0.125
- expert_down: bfloat16 [32, 6144, 2048], P('ep', 'tp'), may hold values from -0.078125 to 0.078125
Outputs:
- mixer_out: bfloat16 [16384, 2048], P(('ep', 'tp'))
- moe_out: bfloat16 [16384, 2048], P(('ep', 'tp'))
The draws below stay inside these ranges and needn't reach their ends.
Inputs may be any that keep to these rules, and one draw needn't show every extreme that they name: `routes`: each row names 2 different experts. Among the rows of one device no expert is named by more than 12 rows, a bound that some blocks reach.
All inputs are finite; a program needn't handle non-finite values.
Results may differ from the reference program's by a relative error of at most 0.012.
Values may be sent and summed in bfloat16 or wider, within the bound.
No kernel may reach another device: no remote copies, remote signals or barrier semaphores. Data moves between devices by JAX's collectives and lax.ppermute only.
A program may use at most 128 MiB of HBM per device.

```python
import math
import jax
import jax.numpy as jnp
import numpy as np
from jax import lax

D = 2048
CW = 1024
FFE = 6144
TOP = 2
TOK_DEV = 128
EXPERTS = 32
CAP = 12
TOKENS_A = 16384
TOKENS_B = 16384
N_TP = 4


def levels(own_key, dims, cuts, smallest, largest):
    level = 1.0
    for axis_at, blocks in cuts:
        heights = jax.random.uniform(jax.random.fold_in(jax.random.fold_in(own_key, 6), axis_at), (blocks,), jnp.float32, smallest / len(cuts), largest / len(cuts))
        level = level * jnp.repeat(jnp.exp(heights), dims[axis_at] // blocks).reshape((-1,) + (1,) * (len(dims) - 1 - axis_at))
    return level


def shared_out(stream_key, own, number, rows, amount, top, most, lean):
    order = jax.random.permutation(stream_key, amount)
    packed, usual = load_shares(amount, rows * top, most, lean, True), load_shares(amount, rows * top, most, lean, False)
    places = jnp.arange(amount)

    def named(tallies, rotation):
        used = int((tallies > 0).sum())
        fixed = max(1, used // 4)
        moved = fixed + (places - fixed + rotation * (used - fixed)) % max(1, amount - fixed)
        return jnp.zeros((amount,), jnp.int32).at[order[jnp.where(places < fixed, places, moved)]].set(jnp.asarray(tallies, jnp.int32))

    tallies = jnp.where(number % 4 == 0, named(packed, number // 4), named(usual, number - number // 4 - 1))
    mixed = jax.random.permutation(jax.random.fold_in(own, 3), amount)
    donor, sink = mixed[0:amount // 2 * 2:2], mixed[1:amount // 2 * 2:2]
    margin = jnp.minimum(tallies[donor] - 1, most - tallies[sink]) // 2
    margin = jnp.where((donor == order[0]) | (sink == order[0]) | (tallies[sink] == 0), 0, jnp.maximum(margin, 0))
    moved = jax.random.randint(jax.random.fold_in(own, 4), (amount // 2,), 0, 1 << 20) % (margin + 1)
    tallies = tallies.at[donor].add(-moved).at[sink].add(moved)
    labels = jnp.searchsorted(jnp.cumsum(tallies), jnp.arange(rows * top), side="right").astype(jnp.int32)
    listing = labels.reshape(top, rows).T
    listing = listing[jax.random.permutation(jax.random.fold_in(own, 1), rows)]
    rotation = jax.random.randint(jax.random.fold_in(own, 2), (rows, 1), 0, top)
    return jnp.take_along_axis(listing, (jnp.arange(top)[None, :] + rotation) % top, axis=1)


def load_shares(number_of, total, reach, skew, full):
    loads = [(1 << 20) // math.isqrt(standing ** skew) + 1 for standing in range(1, number_of + 1)]
    largest = reach if full else min(reach, max(-(-total // number_of), total * loads[0] // sum(loads)))
    least = 1 if total - largest >= number_of - 1 else 0
    holding, spare = [largest] + [least] * (number_of - 1), total - largest - least * (number_of - 1)
    while spare > 0:
        candidates = [i for i in range(1, number_of) if holding[i] < largest] or [i for i in range(1, number_of) if holding[i] < reach]
        whole, budget = sum([loads[i] for i in candidates]), spare
        for i in candidates:
            more = min(reach - holding[i], max(1, budget * loads[i] // whole), spare)
            holding[i] = holding[i] + more
            spare = spare - more
    return np.array(holding)


def scatter_about(own_key, shape, deviation, bound, pieces=(), kind=jnp.bfloat16):
    loudness = levels(own_key, shape, pieces, -0.22, 0.18) if pieces else 1.0
    drawn = jax.random.normal(own_key, shape, jnp.float32) * deviation * loudness
    return jnp.minimum(jnp.maximum(drawn, -bound), bound).astype(kind)


def setup_inputs(seed: int = 0) -> dict:
    key_list = jax.random.split(jax.random.key(seed), 13)
    value_in = scatter_about(key_list[0], (TOKENS_A, CW), 1.0, 6.0, ((0, 32), (1, 4)))
    gate_in = scatter_about(key_list[1], (TOKENS_A, CW), 1.0, 6.0, ((0, 32), (1, 4)))
    outer_gate = scatter_about(key_list[2], (TOKENS_A, CW), 1.0, 6.0, ((0, 32), (1, 4)))
    conv_weight = scatter_about(key_list[3], (3, CW), 3 ** -0.5, 3.5, ((1, 4),))
    out_weight = scatter_about(key_list[4], (CW, D), CW ** -0.5, 0.1875, ((0, 4),))
    moe_tokens = scatter_about(key_list[5], (TOKENS_B, D), 1.0, 6.0, ((0, 128),))
    norm_gain = jnp.clip(1.0 + 0.18 * jax.random.normal(key_list[6], (D,), jnp.float32), 0.099609375, 1.8984375).astype(jnp.bfloat16)
    routes_keys = jax.random.split(jax.random.fold_in(key_list[7], 1), TOKENS_B // TOK_DEV)
    routes_turns = jax.random.permutation(jax.random.fold_in(key_list[7], 3), TOKENS_B // TOK_DEV)
    routes = jax.vmap(lambda own, number: shared_out(jax.random.fold_in(key_list[7], 2), own, number, TOK_DEV, EXPERTS, TOP, CAP, 2))(routes_keys, routes_turns).reshape((TOKENS_B, TOP))
    route_weight = jnp.clip(0.1 + 0.9 * jax.random.uniform(key_list[8], (TOKENS_B, TOP), jnp.float32) ** levels(key_list[8], (TOKENS_B, TOP), ((0, 128),), -0.2, 0.2), 0.1, 1.0)
    expert_gate = scatter_about(key_list[9], (EXPERTS, D, FFE), D ** -0.5, 0.125, ((0, 32), (2, 4)))
    expert_up = scatter_about(key_list[10], (EXPERTS, D, FFE), D ** -0.5, 0.125, ((0, 32), (2, 4)))
    expert_down = scatter_about(key_list[11], (EXPERTS, FFE, D), FFE ** -0.5, 0.078125, ((0, 32), (1, 4)))
    return {"value_in": value_in, "gate_in": gate_in, "outer_gate": outer_gate, "conv_weight": conv_weight, "out_weight": out_weight, "moe_tokens": moe_tokens, "norm_gain": norm_gain, "routes": routes, "route_weight": route_weight, "expert_gate": expert_gate, "expert_up": expert_up, "expert_down": expert_down}


def rounded(values):
    return lax.optimization_barrier(values.astype(jnp.bfloat16)).astype(jnp.float32)

def reference(value_in, gate_in, outer_gate, conv_weight, out_weight, moe_tokens, norm_gain, routes, route_weight, expert_gate, expert_up, expert_down):
    product = (value_in.astype(jnp.float32) * gate_in.astype(jnp.float32)).astype(jnp.bfloat16)
    padded = jnp.pad(product.astype(jnp.float32), ((1, 1), (0, 0)))
    taps = conv_weight.astype(jnp.float32)
    convolved = padded[:-2] * taps[0] + padded[1:-1] * taps[1] + padded[2:] * taps[2]
    mixed_rows = (outer_gate.astype(jnp.float32) * convolved).astype(jnp.bfloat16)
    group_width = CW // N_TP
    running = jnp.zeros((TOKENS_A, D), jnp.float32)
    for group in range(N_TP):
        partial_value = jnp.dot(mixed_rows[:, group * group_width:(group + 1) * group_width], out_weight[group * group_width:(group + 1) * group_width], preferred_element_type=jnp.float32)
        running = running + rounded(partial_value)
    mixer_out = running.astype(jnp.bfloat16)
    tokens_f32 = moe_tokens.astype(jnp.float32)
    normed = (tokens_f32 * lax.rsqrt(lax.optimization_barrier(jnp.mean(tokens_f32 * tokens_f32, axis=-1, keepdims=True)) + 1e-06) * norm_gain.astype(jnp.float32)).astype(jnp.bfloat16)
    devices = TOKENS_B // TOK_DEV
    flat_ids = routes.reshape(devices, TOK_DEV * TOP)
    matches = (flat_ids[..., None] == jnp.arange(EXPERTS, dtype=jnp.int32)[None, None, :]).astype(jnp.int32)
    position = lax.optimization_barrier(jnp.sum((jnp.cumsum(matches, axis=1) - 1) * matches, axis=-1)).astype(jnp.int32)
    owners = jnp.arange(devices, dtype=jnp.int32)[:, None]
    columns = (owners * CAP + position).astype(jnp.int32)
    token_ids = jnp.broadcast_to(jnp.arange(TOKENS_B, dtype=jnp.int32).reshape(devices, TOK_DEV, 1), (devices, TOK_DEV, TOP)).reshape(devices, TOK_DEV * TOP)
    slot_table = jnp.zeros((EXPERTS, devices * CAP), jnp.int32).at[flat_ids, columns].set(token_ids + 1)
    padded_rows = jnp.concatenate([jnp.zeros((1, D), jnp.bfloat16), normed], axis=0)
    unit_width = FFE // N_TP

    def expert(operands):
        indices, gate_w, up_w, down_w = operands
        picked_rows = padded_rows[indices]
        gate_act = jnp.dot(picked_rows, gate_w, preferred_element_type=jnp.float32)
        up_act = jnp.dot(picked_rows, up_w, preferred_element_type=jnp.float32)
        hidden = (jax.nn.silu(gate_act) * up_act).astype(jnp.bfloat16)
        summed = jnp.zeros((indices.shape[0], D), jnp.float32)
        for group in range(N_TP):
            partial_value = jnp.dot(hidden[:, group * unit_width:(group + 1) * unit_width], down_w[group * unit_width:(group + 1) * unit_width], preferred_element_type=jnp.float32)
            summed = summed + rounded(partial_value)
        return summed.astype(jnp.bfloat16)
    results = lax.map(expert, (slot_table, expert_gate, expert_up, expert_down))
    where_ids = (flat_ids * (devices * CAP) + columns).reshape(TOKENS_B, TOP)
    picked = results.reshape(EXPERTS * devices * CAP, D)[where_ids].astype(jnp.float32)
    moe_out = lax.optimization_barrier(jnp.sum(route_weight[..., None] * picked, axis=1)).astype(jnp.bfloat16)
    return (mixer_out, moe_out)
```

```python
import functools

import jax
import jax.numpy as jnp
from jax import lax
from jax.experimental import pallas as pl
from jax.experimental.pallas import tpu as pltpu
from jax.sharding import Mesh
from jax.sharding import PartitionSpec as P

EP = ("ep_0", "ep_1", "ep_2")
EP_TP = ("ep_0", "ep_1", "ep_2", "tp")
ZY = ("ep_0", "ep_1")
CHUNKS = ((0, 8), (8, 24))
F32 = jnp.float32
BF16 = jnp.bfloat16


def shift(x, axis, by):
    size = lax.axis_size(axis)
    return lax.ppermute(x, axis, [(i, (i + by) % size) for i in range(size)])


def neighbours(product):
    size = lax.axis_size(EP)
    up = [(i, i + 1) for i in range(size - 1)]
    down = [(j, i) for i, j in up]
    rows = product.shape[0]
    before = lax.ppermute(product[rows - 1 :], EP, up)
    after = lax.ppermute(product[:1], EP, down)
    return before, after


def mixer_rows(value_in, gate_in, outer_gate, conv_weight, out_weight):
    product = (value_in.astype(F32) * gate_in.astype(F32)).astype(BF16)
    before, after = neighbours(product)
    padded = jnp.concatenate([before, product, after], axis=0).astype(F32)
    taps = conv_weight.astype(F32)
    convolved = padded[:-2] * taps[0] + padded[1:-1] * taps[1] + padded[2:] * taps[2]
    mixed_rows = (outer_gate.astype(F32) * convolved).astype(BF16)
    partial = jnp.dot(mixed_rows, out_weight, preferred_element_type=F32).astype(BF16)
    return partial


def mixer_sum(partial):
    tp = lax.axis_size("tp")
    rows, width = partial.shape
    parts = partial.reshape(tp, rows // tp, width)
    parts = lax.all_to_all(parts, "tp", 0, 0, tiled=True)
    return jnp.sum(parts.astype(F32), axis=0).astype(BF16)


def slots_of(routes, core, groups):
    tokens = routes.shape[1]
    mine = (2 * lax.broadcasted_iota(jnp.int32, (groups, tokens), 0) + core).astype(F32)
    match = [jnp.where(routes[k : k + 1] == mine, 1.0, 0.0) for k in range(routes.shape[0])]
    every = sum(match)
    before = lax.broadcasted_iota(jnp.int32, (tokens, tokens), 0)
    after = lax.broadcasted_iota(jnp.int32, (tokens, tokens), 1)
    upper = jnp.where(before < after, 1.0, 0.0).astype(BF16)
    slot = jnp.dot(every.astype(BF16), upper, preferred_element_type=F32)
    return match, every, jnp.where(every > 0.5, slot, -1.0)


def one_hot_rows(value, slot, first, last):
    groups, tokens = slot.shape
    rows = []
    for g in range(groups):
        names = first + lax.broadcasted_iota(jnp.int32, (last - first, tokens), 0)
        rows.append(jnp.where(slot[g : g + 1] == names.astype(F32), value[g : g + 1], 0.0))
    return jnp.concatenate(rows, axis=0)


def dispatch_body(core_ref, own_ref, other_ref, routes_ref, gain_ref, *out_refs):
    groups = 16
    tokens = jnp.concatenate([own_ref[...], other_ref[...]], axis=0).astype(F32)
    scale = lax.rsqrt(jnp.mean(tokens * tokens, axis=-1, keepdims=True) + 1e-06)
    normed = (tokens * scale * gain_ref[...].astype(F32)).astype(BF16)
    _, every, slot = slots_of(routes_ref[...], core_ref[0], groups)
    for (first, last), out_ref in zip(CHUNKS, out_refs):
        hot = one_hot_rows(every, slot, first, last).astype(BF16)
        out_ref[...] = jnp.dot(hot, normed, preferred_element_type=F32).astype(BF16)


def weights_body(core_ref, routes_ref, weight_ref, *out_refs):
    groups = 16
    match, _, slot = slots_of(routes_ref[...], core_ref[0], groups)
    value = sum(m * weight_ref[k : k + 1] for k, m in enumerate(match))
    for (first, last), out_ref in zip(CHUNKS, out_refs):
        hot = one_hot_rows(value, slot, first, last)
        turned = jnp.transpose(hot)
        high = turned.astype(BF16)
        low = (turned - high.astype(F32)).astype(BF16)
        out_ref[0] = high
        out_ref[1] = low


def combine_first_body(weight_ref, rows_ref, out_ref):
    rows = rows_ref[...]
    total = jnp.dot(weight_ref[0], rows, preferred_element_type=F32)
    out_ref[...] = total + jnp.dot(weight_ref[1], rows, preferred_element_type=F32)


def combine_last_body(weight_ref, rows_ref, before_ref, own_ref, other_ref):
    rows = rows_ref[...]
    total = jnp.dot(weight_ref[0], rows, preferred_element_type=F32)
    total = total + jnp.dot(weight_ref[1], rows, preferred_element_type=F32) + before_ref[...]
    half = own_ref.shape[0]
    own_ref[...] = total[:half]
    other_ref[...] = total[half:].astype(BF16)


def small_call(body, outs, *args, scalars=0, name=None):
    specs = [pl.BlockSpec(memory_space=pltpu.SMEM)] * scalars
    specs += [pl.BlockSpec(memory_space=pltpu.VMEM)] * (len(args) - scalars)
    return pl.pallas_call(
        body,
        out_shape=outs,
        in_specs=specs,
        out_specs=jax.tree.map(lambda _: pl.BlockSpec(memory_space=pltpu.VMEM), outs),
        name=name,
        cost_estimate=pl.CostEstimate(flops=2_000_000_000, bytes_accessed=4_000_000, transcendentals=0),
    )(*args)


def ffn_body(*refs, pieces, steps):
    x_refs = refs[:pieces]
    gate_ref, up_ref, down_ref = refs[pieces : pieces + 3]
    out_refs = refs[pieces + 3 : 2 * pieces + 3]
    total_ref = refs[-1]
    step = pl.program_id(0)
    rows = jnp.concatenate([r[...] for r in x_refs], axis=0)
    gate = jnp.dot(rows, gate_ref[0], preferred_element_type=F32)
    up = jnp.dot(rows, up_ref[0], preferred_element_type=F32)
    hidden = (gate / (1.0 + jnp.exp(-gate)) * up).astype(BF16)
    part = jnp.dot(hidden, down_ref[0], preferred_element_type=F32)

    @pl.when(step == 0)
    def _():
        total_ref[...] = part

    @pl.when(jnp.logical_and(step > 0, step < steps - 1))
    def _():
        total_ref[...] += part

    @pl.when(step == steps - 1)
    def _():
        total = (total_ref[...] + part).astype(BF16)
        at = 0
        for out_ref in out_refs:
            count = out_ref.shape[0]
            out_ref[...] = total[at : at + count]
            at += count


def ffn(xs, gate, up, down, name, block=512):
    width, units = gate.shape[1:]
    steps = units // block
    rows = sum(x.shape[0] for x in xs)
    whole = [pl.BlockSpec(x.shape, lambda j: (0, 0)) for x in xs]
    return pl.pallas_call(
        functools.partial(ffn_body, pieces=len(xs), steps=steps),
        grid=(steps,),
        in_specs=whole
        + [
            pl.BlockSpec((1, width, block), lambda j: (0, 0, j)),
            pl.BlockSpec((1, width, block), lambda j: (0, 0, j)),
            pl.BlockSpec((1, block, width), lambda j: (0, j, 0)),
        ],
        out_specs=whole,
        out_shape=[jax.ShapeDtypeStruct(x.shape, BF16) for x in xs],
        scratch_shapes=[pltpu.VMEM((rows, width), F32)],
        compiler_params=pltpu.CompilerParams(vmem_limit_bytes=56 * 1024 * 1024),
        cost_estimate=pl.CostEstimate(
            flops=6 * rows * width * units, bytes_accessed=3 * 2 * width * units, transcendentals=rows * units
        ),
        name=name,
    )(*xs, gate, up, down)


def gather_over_x(x):
    half = x.shape[0] // 2
    left = shift(x, "tp", 1)
    right = shift(x, "tp", -1)
    far_top = shift(left[:half], "tp", 1)
    far_low = shift(right[half:], "tp", -1)
    return left, right, far_top, far_low


def scatter_over_x(own, left, right, far_top, far_low):
    half = far_top.shape[0]
    top = shift(far_top, "tp", 1)
    low = shift(far_low, "tp", -1)
    right_sum = jnp.concatenate([(right[:half].astype(F32) + top.astype(F32)).astype(BF16), right[half:]], axis=0)
    left_sum = jnp.concatenate([left[:half], (left[half:].astype(F32) + low.astype(F32)).astype(BF16)], axis=0)
    from_left = shift(right_sum, "tp", 1)
    from_right = shift(left_sum, "tp", -1)
    return (own.astype(F32) + from_left.astype(F32) + from_right.astype(F32)).astype(BF16)


def over_zy(x):
    count = lax.axis_size(ZY)
    blocks = x.reshape(count, x.shape[0] // count, x.shape[1])
    return lax.all_to_all(blocks, ZY, 0, 0, tiled=True).reshape(x.shape)


def body(
    value_in,
    gate_in,
    outer_gate,
    conv_weight,
    out_weight,
    moe_tokens,
    norm_gain,
    routes,
    route_weight,
    expert_gate,
    expert_up,
    expert_down,
):
    own_rows, width = moe_tokens.shape
    groups = lax.axis_size(ZY)
    core = lax.axis_index("ep_2").astype(jnp.int32).reshape(1)
    facts = jnp.concatenate([routes.T.astype(F32), route_weight.T], axis=0)
    other_facts = shift(facts, "ep_2", 1)
    other_tokens = shift(moe_tokens, "ep_2", 1)
    both = jnp.concatenate([facts, other_facts], axis=1)
    top = routes.shape[1]
    outgoing = small_call(
        dispatch_body,
        [jax.ShapeDtypeStruct((groups * (b - a), width), BF16) for a, b in CHUNKS],
        core,
        moe_tokens,
        other_tokens,
        both[:top],
        norm_gain.reshape(1, width),
        scalars=1,
        name="dispatch",
    )
    arrived = [over_zy(x) for x in outgoing]
    partial = mixer_rows(value_in, gate_in, outer_gate, conv_weight, out_weight)
    mixer_out = mixer_sum(partial)
    weights = small_call(
        weights_body,
        [jax.ShapeDtypeStruct((2, 2 * own_rows, groups * (b - a)), BF16) for a, b in CHUNKS],
        core,
        both[:top],
        both[top:],
        scalars=1,
        name="weights",
    )
    summed = []
    for c, x in enumerate(arrived):
        left, right, far_top, far_low = gather_over_x(x)
        if c == 0:
            parts = ffn([x, left, right, far_top, far_low], expert_gate, expert_up, expert_down, f"ffn_{c}")
        else:
            near = ffn([x, left, right], expert_gate, expert_up, expert_down, f"ffn_near_{c}")
            far = ffn([far_top, far_low], expert_gate, expert_up, expert_down, f"ffn_far_{c}")
            parts = list(near) + list(far)
        summed.append(scatter_over_x(*parts))
    returned = [over_zy(x) for x in summed]
    first = small_call(
        combine_first_body,
        jax.ShapeDtypeStruct((2 * own_rows, width), F32),
        weights[0],
        returned[0],
        name="combine_first",
    )
    own, other = small_call(
        combine_last_body,
        [jax.ShapeDtypeStruct((own_rows, width), F32), jax.ShapeDtypeStruct((own_rows, width), BF16)],
        weights[1],
        returned[1],
        first,
        name="combine_last",
    )
    moe_out = (own + shift(other, "ep_2", 1).astype(F32)).astype(BF16)
    return (mixer_out, moe_out)


def solution(mesh):
    torus = Mesh(mesh.devices.reshape(4, 4, 2, mesh.shape["tp"]), ("ep_0", "ep_1", "ep_2", "tp"))
    placed = (
        P(EP, "tp"),
        P(EP, "tp"),
        P(EP, "tp"),
        P(None, "tp"),
        P("tp", None),
        P(EP_TP, None),
        P(),
        P(EP_TP, None),
        P(EP_TP, None),
        P(EP, None, "tp"),
        P(EP, None, "tp"),
        P(EP, "tp", None),
    )
    return jax.shard_map(
        body,
        mesh=torus,
        in_specs=placed,
        out_specs=(P(EP_TP, None), P(EP_TP, None)),
        check_vma=False,
    )
```
